32 devices in a mesh: sp: 8 (over z, core), tp: 4 (over y, x).
Axes of the slice: x: 2, y: 2, z: 4, core: 2. Of those that a mesh axis runs over, the one named last changes fastest.
Arguments:
- moe_input: bfloat16 [2048, 2048], P('sp', 'tp'), may hold values from -6 to 6
- out_grad: bfloat16 [2048, 2048], P('sp', 'tp'), may hold values from -8 to 8
- routes: int32 [2048, 2], P('sp'), may hold values from 0 to 7, all different within a row; in each aligned block of 256 rows (0 to 255, 256 to 511, ...) at most 80 rows name the same one
- route_weight: float32 [2048, 2], P('sp'), may hold values from 0.2 to 1.5
- w_gate: bfloat16 [8, 2048, 2048], P('sp', None, 'tp'), may hold values from -0.125 to 0.125
- w_up: bfloat16 [8, 2048, 2048], P('sp', None, 'tp'), may hold values from -0.125 to 0.125
- w_down: bfloat16 [8, 2048, 2048], P('sp', 'tp'), may hold values from -0.125 to 0.125
- w_out: bfloat16 [2048, 2048], P(None, 'tp'), may hold values from -0.125 to 0.125
- queries: bfloat16 [2048, 1024], P('sp', 'tp'), may hold values from -6 to 6
- key_rows: bfloat16 [2048, 1024], P('sp', 'tp'), may hold values from -6 to 6
- value_rows: bfloat16 [2048, 2048], P('sp', 'tp'), may hold values from -6 to 6
- log_decay: float32 [2048, 1024], P('sp', 'tp'), may hold values from -1 to 0
Outputs:
- grad_gate: bfloat16 [8, 2048, 2048], P('sp', None, 'tp')
- grad_up: bfloat16 [8, 2048, 2048], P('sp', None, 'tp')
- grad_down: bfloat16 [8, 2048, 2048], P('sp', 'tp')
- grad_proj: float32 [2048, 2048], P('sp', 'tp')
- grad_queries: bfloat16 [2048, 1024], P('sp', 'tp')
- grad_keys: bfloat16 [2048, 1024], P('sp', 'tp')
- grad_values: bfloat16 [2048, 2048], P('sp', 'tp')
- grad_decay: float32 [2048, 1024], P('sp', 'tp')
The draws below stay inside these ranges and needn't reach their ends.
Inputs may be any that keep to these rules, and one draw needn't show every extreme that they name: `routes`: A token's experts differ. Within each aligned block of 256 tokens no expert is named more than 80 times, and in some block one expert is named exactly 80 times.
All inputs are finite; a program needn't handle non-finite values.
Results may differ from the reference program's by a relative error of at most 0.025.
Values may be sent and summed in bfloat16 or wider, within the bound.
A program may use at most 64 MiB of HBM per device.

```python
import math
import jax
import jax.numpy as jnp
import numpy as np
from jax import lax

D = 2048
HEAD_COUNT = 32
KEY_CHANNELS = 32
VAL_DIM = 64
EXP_HIDDEN = 2048
TOP = 2
BLOCK = 64
TOK_DEV = 256
TOKEN_COUNT = 2048
EXPERTS = 8
CAP = 80
HID_DEV = 512
N_SP = 8
N_TP = 4


def draw_log_decay(key, part):
    sequence_lanes = jax.random.split(jax.random.fold_in(key, 17), 5)
    lagging_head = jax.random.uniform(sequence_lanes[0], (HEAD_COUNT,), jnp.float32) < 0.5
    base_rate = jnp.where(lagging_head, 0.5 / TOKEN_COUNT, 1.0 / 40.0)
    spans = TOKEN_COUNT // TOK_DEV
    span_scale = jnp.exp(jax.random.uniform(sequence_lanes[1], (spans,), jnp.float32, -0.7, 0.7))
    position_scale = jnp.repeat(span_scale, TOK_DEV)
    wobble = jnp.exp(jax.random.uniform(sequence_lanes[2], (TOKEN_COUNT, HEAD_COUNT, KEY_CHANNELS), jnp.float32, -1.0, 1.0))
    smoothed_decay = -(position_scale[:, None, None] * base_rate[None, :, None] * wobble)
    spike_position = jax.random.randint(sequence_lanes[3], (2,), 0, TOKEN_COUNT)
    spike_length = jnp.log(jax.random.uniform(sequence_lanes[4], (2,), jnp.float32, 0.5, 0.8))
    spike_rows = jnp.sum(jnp.where(jnp.arange(TOKEN_COUNT)[:, None] == spike_position[None, :], spike_length[None, :], 0.0), axis=1)
    spike_addend = spike_rows[:, None, None] * lagging_head[None, :, None].astype(jnp.float32)
    return (smoothed_decay + spike_addend).reshape(TOKEN_COUNT, HEAD_COUNT * KEY_CHANNELS)


def raised(entries, key, source, target, parts, factor):
    owner, partner = [(jnp.arange(entries.shape[axis_at]) // (entries.shape[axis_at] // parts)).reshape([-1 if axis == axis_at else 1 for axis in range(entries.ndim)]) for axis_at in (source, target)]
    chosen = jax.random.permutation(key, parts)[partner]
    strong = (owner == chosen) | (owner == (partner + parts // 2) % parts)
    return jnp.where(strong, factor * entries, entries)


def shard_levels(rng, shape, shards, low, top_value):
    gain, own = 1.0, jax.random.fold_in(rng, 6)
    for dim, blocks in shards:
        heights = jnp.exp(jax.random.uniform(jax.random.fold_in(own, dim), (blocks,), jnp.float32, low / len(shards), top_value / len(shards)))
        gain = gain * jnp.repeat(heights, shape[dim] // blocks).reshape([-1 if axis == dim else 1 for axis in range(len(shape))])
    return gain


def shared_out(own_key, own, number, rows, amount, top, reach, lean):
    ranking = jax.random.permutation(own_key, amount)
    crowded, ordinary = shares(amount, rows * top, reach, lean, True), shares(amount, rows * top, reach, lean, False)
    places = jnp.arange(amount)

    def named(tallies, rotation):
        used = int((tallies > 0).sum())
        fixed = max(1, used // 4)
        passed = fixed + (places - fixed + rotation * (used - fixed)) % max(1, amount - fixed)
        return jnp.zeros((amount,), jnp.int32).at[ranking[jnp.where(places < fixed, places, passed)]].set(jnp.asarray(tallies, jnp.int32))

    tallies = jnp.where(number % 4 == 0, named(crowded, number // 4), named(ordinary, number - number // 4 - 1))
    mixed = jax.random.permutation(jax.random.fold_in(own, 3), amount)
    giver, taker = mixed[0:amount // 2 * 2:2], mixed[1:amount // 2 * 2:2]
    room = jnp.minimum(tallies[giver] - 1, reach - tallies[taker]) // 2
    room = jnp.where((giver == ranking[0]) | (taker == ranking[0]) | (tallies[taker] == 0), 0, jnp.maximum(room, 0))
    passed = jax.random.randint(jax.random.fold_in(own, 4), (amount // 2,), 0, 1 << 20) % (room + 1)
    tallies = tallies.at[giver].add(-passed).at[taker].add(passed)
    labels = jnp.searchsorted(jnp.cumsum(tallies), jnp.arange(rows * top), side="right").astype(jnp.int32)
    table = labels.reshape(top, rows).T
    table = table[jax.random.permutation(jax.random.fold_in(own, 1), rows)]
    rotation = jax.random.randint(jax.random.fold_in(own, 2), (rows, 1), 0, top)
    return jnp.take_along_axis(table, (jnp.arange(top)[None, :] + rotation) % top, axis=1)


def shares(count, total, limit, skew, full):
    weights = [(1 << 20) // math.isqrt(rank ** skew) + 1 for rank in range(1, count + 1)]
    largest = limit if full else min(limit, max(-(-total // count), total * weights[0] // sum(weights)))
    least = 1 if total - largest >= count - 1 else 0
    given, spare = [largest] + [least] * (count - 1), total - largest - least * (count - 1)
    while spare > 0:
        candidates = [i for i in range(1, count) if given[i] < largest] or [i for i in range(1, count) if given[i] < limit]
        pool, left = sum([weights[i] for i in candidates]), spare
        for i in candidates:
            addition = min(limit - given[i], max(1, left * weights[i] // pool), spare)
            given[i] = given[i] + addition
            spare = spare - addition
    return np.array(given)


def gaussian(key, shape, spread, limit, cuts=(), kind=jnp.bfloat16):
    entries = spread * jax.random.normal(key, shape, jnp.float32)
    if cuts:
        entries = entries * shard_levels(key, shape, cuts, -0.22, 0.18)
    return jnp.clip(entries, -limit, limit).astype(kind)


def bell_draw_with(key, dims, width, limit, cuts, heavy, held_as=jnp.bfloat16):
    entries = width * jax.random.normal(key, dims, jnp.float32)
    if cuts:
        entries = entries * shard_levels(key, dims, cuts, -0.22, 0.18)
    return jnp.clip(raised(entries, jax.random.fold_in(key, 3), *heavy), -limit, limit).astype(held_as)


def setup_inputs(seed: int = 0) -> dict:
    splits = jax.random.split(jax.random.key(seed), 13)
    moe_input = gaussian(splits[0], (TOKEN_COUNT, D), 1.0, 6.0, ((0, 8), (1, 4)))
    out_grad = bell_draw_with(splits[1], (TOKEN_COUNT, D), 1.0, 8.0, ((0, 8), (1, 4)), (0, 1, 8, 2.0))
    routes_keys = jax.random.split(jax.random.fold_in(splits[2], 1), TOKEN_COUNT // TOK_DEV)
    routes_turns = jax.random.permutation(jax.random.fold_in(splits[2], 3), TOKEN_COUNT // TOK_DEV)
    routes = jax.vmap(lambda own, number: shared_out(jax.random.fold_in(splits[2], 2), own, number, TOK_DEV, EXPERTS, TOP, CAP, 2))(routes_keys, routes_turns).reshape((TOKEN_COUNT, TOP))
    route_weight = jnp.clip(0.2 + 1.3 * jax.random.uniform(splits[3], (TOKEN_COUNT, TOP), jnp.float32) ** shard_levels(splits[3], (TOKEN_COUNT, TOP), ((0, 8),), -0.2, 0.2), 0.2, 1.5)
    w_gate = gaussian(splits[4], (EXPERTS, D, EXP_HIDDEN), D ** -0.5, 0.125, ((0, 8), (2, 4)))
    w_up = gaussian(splits[5], (EXPERTS, D, EXP_HIDDEN), D ** -0.5, 0.125, ((0, 8), (2, 4)))
    w_down = gaussian(splits[6], (EXPERTS, EXP_HIDDEN, D), EXP_HIDDEN ** -0.5, 0.125, ((0, 8), (1, 4)))
    w_out = gaussian(splits[7], (D, HEAD_COUNT * VAL_DIM), (HEAD_COUNT * VAL_DIM) ** -0.5, 0.125, ((1, 4),))
    queries = gaussian(splits[8], (TOKEN_COUNT, HEAD_COUNT * KEY_CHANNELS), 1.0, 6.0, ((0, 8), (1, 4)))
    key_rows = gaussian(splits[9], (TOKEN_COUNT, HEAD_COUNT * KEY_CHANNELS), 1.0, 6.0, ((0, 8), (1, 4)))
    value_rows = gaussian(splits[10], (TOKEN_COUNT, HEAD_COUNT * VAL_DIM), 1.0, 6.0, ((0, 8), (1, 4)))
    log_decay = draw_log_decay(jax.random.fold_in(splits[12], 71), 0)
    return {"moe_input": moe_input, "out_grad": out_grad, "routes": routes, "route_weight": route_weight, "w_gate": w_gate, "w_up": w_up, "w_down": w_down, "w_out": w_out, "queries": queries, "key_rows": key_rows, "value_rows": value_rows, "log_decay": log_decay}


PRECISE = lax.Precision.HIGHEST

def mixer_pass(queries, key_rows, value_rows, log_decay, state_in):
    length = queries.shape[0]
    blocks = length // BLOCK
    nheads = state_in.shape[0]
    query_blocks = queries.reshape(blocks, BLOCK, nheads, KEY_CHANNELS)
    key_blocks = key_rows.reshape(blocks, BLOCK, nheads, KEY_CHANNELS) * KEY_CHANNELS ** (-0.5)
    value_blocks = value_rows.reshape(blocks, BLOCK, nheads, VAL_DIM)
    decays = log_decay.reshape(blocks, BLOCK, nheads, KEY_CHANNELS)
    cumulative = jnp.cumsum(decays, axis=1)
    closing = cumulative[:, -1]
    query_scaled = query_blocks * jnp.exp(cumulative)
    key_scaled = key_blocks * jnp.exp(-cumulative)
    causal = jnp.tril(jnp.ones((BLOCK, BLOCK), jnp.float32))
    scores = jnp.einsum('nthd,nshd->nhts', query_scaled, key_scaled, precision=PRECISE) * causal
    within = jnp.einsum('nhts,nshv->nthv', scores, value_blocks, precision=PRECISE)
    key_tail = key_blocks * jnp.exp(closing[:, None] - cumulative)
    additions = jnp.einsum('nshd,nshv->nhdv', key_tail, value_blocks, precision=PRECISE)

    def advance(state_now, pieces):
        return (jnp.exp(pieces[0])[..., None] * state_now + pieces[1], state_now)
    state_out, entering = lax.scan(advance, state_in, (closing, additions))
    carried = jnp.einsum('nthd,nhdv->nthv', query_scaled, entering, precision=PRECISE)
    return ((within + carried).reshape(length, nheads * VAL_DIM), lax.optimization_barrier(jnp.sum(closing, axis=0)), state_out)

def reference(moe_input, out_grad, routes, route_weight, w_gate, w_up, w_down, w_out, queries, key_rows, value_rows, log_decay):
    pair_count = TOKEN_COUNT * TOP
    weighted = (route_weight[:, :, None] * out_grad[:, None, :].astype(jnp.float32)).astype(jnp.bfloat16)
    grad_pad = jnp.concatenate([weighted.reshape(pair_count, D), jnp.zeros((1, D), jnp.bfloat16)], axis=0)
    input_pad = jnp.concatenate([jnp.repeat(moe_input, TOP, axis=0), jnp.zeros((1, D), jnp.bfloat16)], axis=0)
    flat_routes = routes.reshape(N_SP, TOK_DEV * TOP)
    onehot = (flat_routes[:, :, None] == jnp.arange(EXPERTS, dtype=jnp.int32)[None, None, :]).astype(jnp.int32)
    position = lax.optimization_barrier(jnp.sum((jnp.cumsum(onehot, axis=1) - onehot) * onehot, axis=2))
    slot_index = (jnp.arange(N_SP, dtype=jnp.int32)[:, None] * CAP + position).reshape(pair_count)
    slot_table = jnp.full((EXPERTS, N_SP * CAP), pair_count, jnp.int32)
    slot_table = slot_table.at[routes.reshape(pair_count), slot_index].set(jnp.arange(pair_count, dtype=jnp.int32))

    def one_expert(pieces):
        row_index, gate_weight, up_weight, down_weight = pieces
        rows_in = input_pad[row_index]
        rows_grad = grad_pad[row_index]
        gate_pre = jnp.dot(rows_in, gate_weight, preferred_element_type=jnp.float32)
        up_pre = jnp.dot(rows_in, up_weight, preferred_element_type=jnp.float32)
        sigmoid_gate = jax.nn.sigmoid(gate_pre)
        activated = gate_pre * sigmoid_gate
        hidden = (activated * up_pre).astype(jnp.bfloat16)
        hidden_grad = lax.dot_general(rows_grad, down_weight, (((1,), (1,)), ((), ())), preferred_element_type=jnp.float32)
        down_part = lax.dot_general(hidden, rows_grad, (((0,), (0,)), ((), ())), preferred_element_type=jnp.float32).astype(jnp.bfloat16)
        gate_grad = (hidden_grad * up_pre * sigmoid_gate * (1.0 + gate_pre * (1.0 - sigmoid_gate))).astype(jnp.bfloat16)
        up_grad = (hidden_grad * activated).astype(jnp.bfloat16)
        gate_part = lax.dot_general(rows_in, gate_grad, (((0,), (0,)), ((), ())), preferred_element_type=jnp.float32).astype(jnp.bfloat16)
        up_part = lax.dot_general(rows_in, up_grad, (((0,), (0,)), ((), ())), preferred_element_type=jnp.float32).astype(jnp.bfloat16)
        row_total = gate_grad.shape[0]
        gate_split = gate_grad.astype(jnp.float32).reshape(row_total, N_TP, HID_DEV)
        up_split = up_grad.astype(jnp.float32).reshape(row_total, N_TP, HID_DEV)
        gate_wsplit = gate_weight.astype(jnp.float32).reshape(D, N_TP, HID_DEV)
        up_wsplit = up_weight.astype(jnp.float32).reshape(D, N_TP, HID_DEV)
        partial_value = jnp.einsum('rgf,dgf->grd', gate_split, gate_wsplit, precision=PRECISE)
        partial_value = partial_value + jnp.einsum('rgf,dgf->grd', up_split, up_wsplit, precision=PRECISE)
        rounded = lax.optimization_barrier(partial_value.astype(jnp.bfloat16))
        row_grad = lax.optimization_barrier(jnp.sum(rounded.astype(jnp.float32), axis=0))
        return (gate_part, up_part, down_part, row_grad.astype(jnp.bfloat16))
    grad_gate, grad_up, grad_down, returned = lax.map(one_expert, (slot_table, w_gate, w_up, w_down))
    pair_back = jnp.zeros((pair_count + 1, D), jnp.float32)
    pair_back = pair_back.at[slot_table.reshape(-1)].set(returned.reshape(-1, D).astype(jnp.float32))
    routed = lax.optimization_barrier(jnp.sum(pair_back[:pair_count].reshape(TOKEN_COUNT, TOP, D), axis=1))
    residual_grad = (out_grad.astype(jnp.float32) + routed).astype(jnp.bfloat16)
    zero_state = jnp.zeros((HEAD_COUNT, KEY_CHANNELS, VAL_DIM), jnp.float32)

    def mixer_only(query_full, key_full, value_full, decay_full):
        return mixer_pass(query_full, key_full, value_full, decay_full, zero_state)[0]
    mixer_raw, pull_back = jax.vjp(mixer_only, queries.astype(jnp.float32), key_rows.astype(jnp.float32), value_rows.astype(jnp.float32), log_decay)
    mixer_out = mixer_raw.astype(jnp.bfloat16)
    grad_proj = lax.dot_general(residual_grad, mixer_out, (((0,), (0,)), ((), ())), preferred_element_type=jnp.float32)
    mixer_grad = jnp.dot(residual_grad, w_out, preferred_element_type=jnp.float32)
    query_grad, key_grad, value_grad, decay_grad = pull_back(mixer_grad)
    return (grad_gate, grad_up, grad_down, grad_proj, query_grad.astype(jnp.bfloat16), key_grad.astype(jnp.bfloat16), value_grad.astype(jnp.bfloat16), decay_grad)
```

```python
import jax
import jax.numpy as jnp
from jax import lax
from jax.sharding import PartitionSpec as P

KEY_CHANNELS = 32
VAL_DIM = 64
TOP = 2
BLOCK = 64


PRECISE = lax.Precision.HIGHEST


def gathered_spans(log_total, increment):
    rows, width = log_total.size, increment.shape[-1]
    packed = jnp.concatenate([increment.reshape(rows, width), log_total.reshape(-1, width)], axis=0)
    spans = lax.all_gather(packed, "sp")
    return (spans[:, rows:].reshape(-1, rows), spans[:, :rows])


def carried_in(span_logs, span_states, backward):
    count, mine = (lax.axis_size("sp"), lax.axis_index("sp"))
    source = jnp.arange(count)
    if backward:
        between = (source[None, :] < source[:, None]) & (source[None, :] > mine)
        counts = source > mine
    else:
        between = (source[None, :] > source[:, None]) & (source[None, :] < mine)
        counts = source < mine
    logs = jnp.dot(between.astype(jnp.float32), span_logs, precision=PRECISE)
    weights = jnp.where(counts[:, None], jnp.exp(logs), 0.0)
    return jnp.sum(weights[:, :, None] * span_states, axis=0)


def running_sum(values, axis):
    length = values.shape[axis]
    ones = jnp.tril(jnp.ones((length, length), jnp.float32))
    moved = jnp.tensordot(ones, values, axes=((1,), (axis,)), precision=PRECISE)
    return jnp.moveaxis(moved, 0, axis)


def mixer_pass(queries, key_rows, value_rows, log_decay, state_in):
    length = queries.shape[0]
    blocks = length // BLOCK
    nheads = state_in.shape[0]
    query_blocks = queries.reshape(blocks, BLOCK, nheads, KEY_CHANNELS)
    key_blocks = key_rows.reshape(blocks, BLOCK, nheads, KEY_CHANNELS) * KEY_CHANNELS ** (-0.5)
    value_blocks = value_rows.reshape(blocks, BLOCK, nheads, VAL_DIM)
    decays = log_decay.reshape(blocks, BLOCK, nheads, KEY_CHANNELS)
    cumulative = running_sum(decays, 1)
    closing = cumulative[:, -1]
    query_scaled = query_blocks * jnp.exp(cumulative)
    key_scaled = key_blocks * jnp.exp(-cumulative)
    causal = jnp.tril(jnp.ones((BLOCK, BLOCK), jnp.float32))
    scores = jnp.einsum("nthd,nshd->nhts", query_scaled, key_scaled, precision=PRECISE) * causal
    within = jnp.einsum("nhts,nshv->nthv", scores, value_blocks, precision=PRECISE)
    key_tail = key_blocks * jnp.exp(closing[:, None] - cumulative)
    additions = jnp.einsum("nshd,nshv->nhdv", key_tail, value_blocks, precision=PRECISE)

    def advance(state_now, pieces):
        return (jnp.exp(pieces[0])[..., None] * state_now + pieces[1], state_now)

    state_out, entering = lax.scan(advance, state_in, (closing, additions), unroll=True)
    carried = jnp.einsum("nthd,nhdv->nthv", query_scaled, entering, precision=PRECISE)
    return (within + carried).reshape(length, nheads * VAL_DIM)


def carry_terms(key_full, value_full, decay_full):
    length = key_full.shape[0]
    blocks = length // BLOCK
    nheads = key_full.shape[1] // KEY_CHANNELS
    key_blocks = key_full.reshape(blocks, BLOCK, nheads, KEY_CHANNELS) * KEY_CHANNELS ** (-0.5)
    value_blocks = value_full.reshape(blocks, BLOCK, nheads, VAL_DIM)
    cumulative = running_sum(decay_full.reshape(blocks, BLOCK, nheads, KEY_CHANNELS), 1)
    closing = cumulative[:, -1]
    key_tail = key_blocks * jnp.exp(closing[:, None] - cumulative)
    additions = jnp.einsum("nshd,nshv->nhdv", key_tail, value_blocks, precision=PRECISE)
    log_total = jnp.sum(closing, axis=0)
    remaining = log_total[None] - running_sum(closing, 0)
    increment = jnp.einsum("nhd,nhdv->hdv", jnp.exp(remaining), additions, precision=PRECISE)
    return (log_total, increment)


def body(
    moe_input,
    out_grad,
    routes,
    route_weight,
    w_gate,
    w_up,
    w_down,
    w_out,
    queries,
    key_rows,
    value_rows,
    log_decay,
):
    sp_count = lax.axis_size("sp")
    token_count = out_grad.shape[0]
    pair_count = token_count * TOP
    capacity = 5 * token_count * TOP // (4 * sp_count)
    query_full = queries.astype(jnp.float32)
    key_full = key_rows.astype(jnp.float32)
    value_full = value_rows.astype(jnp.float32)
    (log_total, increment), pull_carry = jax.vjp(carry_terms, key_full, value_full, log_decay)
    span_logs, span_states = gathered_spans(log_total, increment)
    state_in = carried_in(span_logs, span_states, False).reshape(increment.shape)
    mixer_raw, pull_mixer = jax.vjp(
        mixer_pass, query_full, key_full, value_full, log_decay, state_in
    )
    mixer_out = mixer_raw.astype(jnp.bfloat16)
    flat_routes = routes.reshape(pair_count)
    onehot = (flat_routes[:, None] == jnp.arange(sp_count, dtype=jnp.int32)[None, :]).astype(
        jnp.int32
    )
    position = jnp.sum((jnp.cumsum(onehot, axis=0) - onehot) * onehot, axis=1)
    pair_slot = flat_routes * capacity + position
    slot_pair = (
        jnp.full((sp_count * capacity,), pair_count, jnp.int32)
        .at[pair_slot]
        .set(jnp.arange(pair_count, dtype=jnp.int32))
    )
    slot_token = slot_pair // TOP
    row_total = sp_count * capacity
    columns = out_grad.shape[1]
    weighted = (route_weight[:, :, None] * out_grad[:, None, :].astype(jnp.float32)).astype(
        jnp.bfloat16
    )
    weighted_pad = jnp.concatenate(
        [weighted.reshape(pair_count, columns), jnp.zeros((1, columns), jnp.bfloat16)], axis=0
    )
    inputs_pad = jnp.concatenate([moe_input, jnp.zeros((1, columns), jnp.bfloat16)], axis=0)
    send_in = jnp.take(inputs_pad, slot_token, axis=0).reshape(sp_count, capacity, columns)
    send_grad = jnp.take(weighted_pad, slot_pair, axis=0).reshape(sp_count, capacity, columns)
    recv_in, recv_grad = (
        lax.all_to_all(send_in, "sp", split_axis=0, concat_axis=0, tiled=True),
        lax.all_to_all(send_grad, "sp", split_axis=0, concat_axis=0, tiled=True),
    )
    rows_in, rows_grad = (
        lax.all_gather(recv_in.reshape(row_total, -1), "tp", axis=1, tiled=True),
        lax.all_gather(recv_grad.reshape(row_total, -1), "tp", axis=1, tiled=True),
    )
    gate_weight = w_gate[0]
    up_weight = w_up[0]
    down_weight = w_down[0]
    gate_pre = jnp.dot(rows_in, gate_weight, preferred_element_type=jnp.float32)
    up_pre = jnp.dot(rows_in, up_weight, preferred_element_type=jnp.float32)
    sigmoid_gate = jax.nn.sigmoid(gate_pre)
    activated = gate_pre * sigmoid_gate
    hidden = (activated * up_pre).astype(jnp.bfloat16)
    hidden_grad = lax.dot_general(
        rows_grad, down_weight, (((1,), (1,)), ((), ())), preferred_element_type=jnp.float32
    )
    down_part = lax.dot_general(
        hidden, rows_grad, (((0,), (0,)), ((), ())), preferred_element_type=jnp.float32
    ).astype(jnp.bfloat16)
    gate_grad = (
        hidden_grad * up_pre * sigmoid_gate * (1.0 + gate_pre * (1.0 - sigmoid_gate))
    ).astype(jnp.bfloat16)
    up_grad = (hidden_grad * activated).astype(jnp.bfloat16)
    gate_part = lax.dot_general(
        rows_in, gate_grad, (((0,), (0,)), ((), ())), preferred_element_type=jnp.float32
    ).astype(jnp.bfloat16)
    up_part = lax.dot_general(
        rows_in, up_grad, (((0,), (0,)), ((), ())), preferred_element_type=jnp.float32
    ).astype(jnp.bfloat16)
    partial_value = lax.dot_general(
        gate_grad, gate_weight, (((1,), (1,)), ((), ())), preferred_element_type=jnp.float32
    )
    partial_value = partial_value + lax.dot_general(
        up_grad, up_weight, (((1,), (1,)), ((), ())), preferred_element_type=jnp.float32
    )
    row_part = lax.psum_scatter(
        partial_value.astype(jnp.bfloat16), "tp", scatter_dimension=1, tiled=True
    )
    back_rows = lax.all_to_all(
        row_part.reshape(sp_count, capacity, -1), "sp", split_axis=0, concat_axis=0, tiled=True
    ).reshape(row_total, -1)
    routed = jnp.sum(
        jnp.take(back_rows, pair_slot, axis=0).astype(jnp.float32).reshape(token_count, TOP, -1),
        axis=1,
    )
    residual_grad = (out_grad.astype(jnp.float32) + routed).astype(jnp.bfloat16)
    full_grad = lax.all_gather(residual_grad, "tp", axis=1, tiled=True)
    grad_proj = lax.psum_scatter(
        lax.dot_general(
            full_grad, mixer_out, (((0,), (0,)), ((), ())), preferred_element_type=jnp.float32
        ).astype(jnp.bfloat16),
        "sp",
        scatter_dimension=0,
        tiled=True,
    ).astype(jnp.float32)
    mixer_grad = jnp.dot(full_grad, w_out, preferred_element_type=jnp.float32)
    query_grad, key_grad, value_grad, decay_grad, state_grad = pull_mixer(mixer_grad)
    span_grads = lax.all_gather(state_grad.reshape(log_total.size, -1), "sp")
    state_out_grad = carried_in(span_logs, span_grads, True).reshape(increment.shape)
    total_grad = jnp.exp(log_total) * jnp.sum(state_out_grad * state_in, axis=2)
    key_extra, value_extra, decay_extra = pull_carry((total_grad, state_out_grad))
    return (
        gate_part[None],
        up_part[None],
        down_part[None],
        grad_proj,
        query_grad.astype(jnp.bfloat16),
        (key_grad + key_extra).astype(jnp.bfloat16),
        (value_grad + value_extra).astype(jnp.bfloat16),
        decay_grad + decay_extra,
    )


def solution(mesh):
    in_specs = (
        P("sp", "tp"),
        P("sp", "tp"),
        P("sp", None),
        P("sp", None),
        P("sp", None, "tp"),
        P("sp", None, "tp"),
        P("sp", "tp", None),
        P(None, "tp"),
        P("sp", "tp"),
        P("sp", "tp"),
        P("sp", "tp"),
        P("sp", "tp"),
    )
    out_specs = (
        P("sp", None, "tp"),
        P("sp", None, "tp"),
        P("sp", "tp", None),
        P("sp", "tp"),
        P("sp", "tp"),
        P("sp", "tp"),
        P("sp", "tp"),
        P("sp", "tp"),
    )
    return jax.shard_map(body, mesh=mesh, in_specs=in_specs, out_specs=out_specs, check_vma=False)
```

```python
import jax
import jax.numpy as jnp
from jax import lax
from jax.experimental import pallas as pl
from jax.experimental.pallas import tpu as pltpu
from jax.sharding import PartitionSpec as P

KEY_CHANNELS = 32
VAL_DIM = 64
TOP = 2
BLOCK = 64


PRECISE = lax.Precision.HIGHEST


SHIFT = 6
LOG_ROWS = 16


def dot_nn(left, right):
    return jnp.dot(left, right, preferred_element_type=jnp.float32)


def dot_nt(left, right):
    return lax.dot_general(left, right, (((1,), (1,)), ((), ())), preferred_element_type=jnp.float32)


def dot_tn(left, right):
    return lax.dot_general(left, right, (((0,), (0,)), ((), ())), preferred_element_type=jnp.float32)


def same_head(rows, columns, column_shift):
    row = lax.shift_right_logical(lax.broadcasted_iota(jnp.int32, (rows, columns), 0), SHIFT)
    column = lax.shift_right_logical(
        lax.broadcasted_iota(jnp.int32, (rows, columns), 1), column_shift
    )
    return jnp.where(row == column, 1.0, 0.0)


def lower_ones():
    row = lax.broadcasted_iota(jnp.int32, (BLOCK, BLOCK), 0)
    column = lax.broadcasted_iota(jnp.int32, (BLOCK, BLOCK), 1)
    return jnp.where(row >= column, 1.0, 0.0)


def causal_ones(columns):
    row = lax.broadcasted_iota(jnp.int32, (BLOCK, columns), 0)
    column = lax.broadcasted_iota(jnp.int32, (BLOCK, columns), 1) & (BLOCK - 1)
    return row >= column


def piled(rows, copies):
    return jnp.concatenate([rows] * copies, axis=0)


def summed(pile, copies):
    total = pile[:BLOCK]
    for index in range(1, copies):
        total = total + pile[index * BLOCK : (index + 1) * BLOCK]
    return total


def running(decay, lower):
    return jnp.dot(lower, decay, precision=PRECISE, preferred_element_type=jnp.float32)


def block_of(ref, index):
    return ref[index * BLOCK : (index + 1) * BLOCK, :]


def scaled_keys(key_ref, index):
    return block_of(key_ref, index).astype(jnp.float32) * KEY_CHANNELS ** (-0.5)


def span_kernel(key_ref, value_ref, decay_ref, out_ref):
    width, values = key_ref.shape[1], value_ref.shape[1]
    lower = lower_ones()
    state = jnp.zeros((values, width), jnp.float32)
    total = jnp.zeros((1, width), jnp.float32)
    for index in range(key_ref.shape[0] // BLOCK):
        cumulative = running(block_of(decay_ref, index), lower)
        closing = cumulative[BLOCK - 1 :]
        tail = (scaled_keys(key_ref, index) * jnp.exp(closing - cumulative)).astype(jnp.bfloat16)
        state = jnp.exp(closing) * state + dot_tn(block_of(value_ref, index), tail)
        total = total + closing
    state = state * same_head(values, width, 5)
    out_ref[:BLOCK, :] = summed(state, values // VAL_DIM).astype(jnp.bfloat16)
    high = total.astype(jnp.bfloat16).astype(jnp.float32)
    middle = (total - high).astype(jnp.bfloat16).astype(jnp.float32)
    low = total - high - middle
    row = lax.broadcasted_iota(jnp.int32, (LOG_ROWS, width), 0)
    logs = jnp.where(row == 0, high, jnp.where(row == 1, middle, low))
    out_ref[BLOCK:, :] = logs.astype(jnp.bfloat16)


def mixer_kernel(query_ref, key_ref, value_ref, decay_ref, state_ref, out_ref):
    width, values = key_ref.shape[1], value_ref.shape[1]
    heads = values // VAL_DIM
    lower = lower_ones()
    key_mask = same_head(values, width, 5)
    key_mask_b = key_mask.astype(jnp.bfloat16)
    value_mask_b = same_head(values, values, SHIFT).astype(jnp.bfloat16)
    causal = causal_ones(values)
    state = piled(state_ref[...], heads) * key_mask
    for index in range(key_ref.shape[0] // BLOCK):
        cumulative = running(block_of(decay_ref, index), lower)
        closing = cumulative[BLOCK - 1 :]
        keys = scaled_keys(key_ref, index)
        value = block_of(value_ref, index)
        query = (block_of(query_ref, index).astype(jnp.float32) * jnp.exp(cumulative)).astype(
            jnp.bfloat16
        )
        key = (keys * jnp.exp(-cumulative)).astype(jnp.bfloat16)
        tail = (keys * jnp.exp(closing - cumulative)).astype(jnp.bfloat16)
        key_pile = piled(key, heads) * key_mask_b
        value_pile = piled(value, heads) * value_mask_b
        scores = jnp.where(causal, dot_nt(query, key_pile), 0.0).astype(jnp.bfloat16)
        mixed = dot_nn(scores, value_pile) + dot_nt(query, state.astype(jnp.bfloat16))
        out_ref[index * BLOCK : (index + 1) * BLOCK, :] = mixed.astype(jnp.bfloat16)
        state = jnp.exp(closing) * state + dot_tn(value, tail) * key_mask


def span_grad_kernel(query_ref, decay_ref, grad_ref, out_ref):
    width, values = query_ref.shape[1], grad_ref.shape[1]
    lower = lower_ones()
    state = jnp.zeros((values, width), jnp.float32)
    for index in reversed(range(query_ref.shape[0] // BLOCK)):
        cumulative = running(block_of(decay_ref, index), lower)
        closing = cumulative[BLOCK - 1 :]
        query = (block_of(query_ref, index).astype(jnp.float32) * jnp.exp(cumulative)).astype(
            jnp.bfloat16
        )
        state = jnp.exp(closing) * state + dot_tn(block_of(grad_ref, index), query)
    state = state * same_head(values, width, 5)
    out_ref[...] = summed(state, values // VAL_DIM).astype(jnp.bfloat16)


def mixer_grad_kernel(
    query_ref,
    key_ref,
    value_ref,
    decay_ref,
    grad_ref,
    state_ref,
    state_grad_ref,
    query_out,
    key_out,
    value_out,
    decay_out,
    entering,
):
    width, values = key_ref.shape[1], value_ref.shape[1]
    heads = values // VAL_DIM
    blocks = key_ref.shape[0] // BLOCK
    lower = lower_ones()
    key_mask = same_head(values, width, 5)
    key_mask_b = key_mask.astype(jnp.bfloat16)
    value_mask = same_head(values, values, SHIFT)
    value_mask_b = value_mask.astype(jnp.bfloat16)
    causal = causal_ones(values)
    state = piled(state_ref[...], heads) * key_mask
    for index in range(blocks):
        entering[index] = state
        if index < blocks - 1:
            cumulative = running(block_of(decay_ref, index), lower)
            closing = cumulative[BLOCK - 1 :]
            tail = (scaled_keys(key_ref, index) * jnp.exp(closing - cumulative)).astype(
                jnp.bfloat16
            )
            state = jnp.exp(closing) * state + dot_tn(block_of(value_ref, index), tail) * key_mask
    state_grad = piled(state_grad_ref[...], heads) * key_mask
    for index in reversed(range(blocks)):
        spot = slice(index * BLOCK, (index + 1) * BLOCK)
        cumulative = running(block_of(decay_ref, index), lower)
        closing = cumulative[BLOCK - 1 :]
        grown, shrunk = (jnp.exp(cumulative), jnp.exp(-cumulative))
        rest = jnp.exp(closing - cumulative)
        keys = scaled_keys(key_ref, index)
        value = block_of(value_ref, index)
        grad = block_of(grad_ref, index)
        query = (block_of(query_ref, index).astype(jnp.float32) * grown).astype(jnp.bfloat16)
        key = (keys * shrunk).astype(jnp.bfloat16)
        tail = (keys * rest).astype(jnp.bfloat16)
        key_pile = piled(key, heads) * key_mask_b
        value_pile = piled(value, heads) * value_mask_b
        scores = jnp.where(causal, dot_nt(query, key_pile), 0.0).astype(jnp.bfloat16)
        score_grad = jnp.where(causal, dot_nt(grad, value_pile), 0.0).astype(jnp.bfloat16)
        state = entering[index]
        leaving = state_grad.astype(jnp.bfloat16)
        query_grad = dot_nn(score_grad, key_pile) + dot_nn(grad, state.astype(jnp.bfloat16))
        key_grad = summed(dot_tn(score_grad, query) * key_mask, heads)
        tail_grad = dot_nn(value, leaving)
        value_grad = summed(dot_tn(scores, grad) * value_mask, heads) + dot_nt(tail, leaving)
        tail_term = tail.astype(jnp.float32) * tail_grad
        inner = (
            query.astype(jnp.float32) * query_grad - key.astype(jnp.float32) * key_grad - tail_term
        )
        faded = jnp.exp(closing) * state_grad
        closing_grad = jnp.sum(tail_term, axis=0, keepdims=True) + jnp.sum(
            faded * state, axis=0, keepdims=True
        )
        later = lax.dot_general(
            lower,
            inner,
            (((0,), (0,)), ((), ())),
            precision=PRECISE,
            preferred_element_type=jnp.float32,
        )
        decay_out[spot, :] = later + closing_grad
        query_out[spot, :] = (query_grad * grown).astype(jnp.bfloat16)
        key_out[spot, :] = (
            (key_grad * shrunk + tail_grad * rest) * KEY_CHANNELS ** (-0.5)
        ).astype(jnp.bfloat16)
        value_out[spot, :] = value_grad.astype(jnp.bfloat16)
        state_grad = faded + dot_tn(grad, query) * key_mask


def local_call(kernel, out_shape, flops, scratch=()):
    return pl.pallas_call(
        kernel,
        out_shape=out_shape,
        scratch_shapes=scratch,
        cost_estimate=pl.CostEstimate(flops=flops, bytes_accessed=1000000, transcendentals=0),
    )


def swapped(pieces, mine):
    bit, count = (1, len(pieces))
    while bit < count:
        swap = (mine & bit) != 0
        pieces = [
            jnp.where(swap, pieces[place ^ bit], pieces[place]) for place in range(count)
        ]
        bit *= 2
    return pieces


def exchanged(rows, step, count):
    return lax.ppermute(rows, "tp", [(place, place ^ step) for place in range(count)])


def gathered_columns(rows):
    count, mine = (lax.axis_size("tp"), lax.axis_index("tp"))
    pieces = [rows] + [exchanged(rows, step, count) for step in range(1, count)]
    return jnp.concatenate(swapped(pieces, mine), axis=1)


def scattered_columns(rows):
    count, mine = (lax.axis_size("tp"), lax.axis_index("tp"))
    width = rows.shape[1] // count
    pieces = swapped([rows[:, place * width : (place + 1) * width] for place in range(count)], mine)
    total = pieces[0].astype(jnp.float32)
    for step in range(1, count):
        total = total + exchanged(pieces[step], step, count).astype(jnp.float32)
    return total.astype(jnp.bfloat16)


def carried_in(span_logs, span_states, backward):
    count, mine = (lax.axis_size("sp"), lax.axis_index("sp"))
    source = jnp.arange(count)
    if backward:
        between = (source[None, :] < source[:, None]) & (source[None, :] > mine)
        counts = source > mine
    else:
        between = (source[None, :] > source[:, None]) & (source[None, :] < mine)
        counts = source < mine
    logs = jnp.dot(between.astype(jnp.float32), span_logs, precision=PRECISE)
    weights = jnp.where(counts[:, None], jnp.exp(logs), 0.0)
    return jnp.sum(weights[:, None, :] * span_states.astype(jnp.float32), axis=0)


def body(
    moe_input,
    out_grad,
    routes,
    route_weight,
    w_gate,
    w_up,
    w_down,
    w_out,
    queries,
    key_rows,
    value_rows,
    log_decay,
):
    sp_count = lax.axis_size("sp")
    token_count = out_grad.shape[0]
    pair_count = token_count * TOP
    capacity = 5 * token_count * TOP // (4 * sp_count)
    flat_routes = routes.reshape(pair_count)
    onehot = (flat_routes[:, None] == jnp.arange(sp_count, dtype=jnp.int32)[None, :]).astype(
        jnp.int32
    )
    position = jnp.sum((jnp.cumsum(onehot, axis=0) - onehot) * onehot, axis=1)
    pair_slot = flat_routes * capacity + position
    slot_pair = (
        jnp.full((sp_count * capacity,), pair_count, jnp.int32)
        .at[pair_slot]
        .set(jnp.arange(pair_count, dtype=jnp.int32))
    )
    slot_token = slot_pair // TOP
    row_total = sp_count * capacity
    columns = out_grad.shape[1]
    weighted = (route_weight[:, :, None] * out_grad[:, None, :].astype(jnp.float32)).astype(
        jnp.bfloat16
    )
    weighted_pad = jnp.concatenate(
        [weighted.reshape(pair_count, columns), jnp.zeros((1, columns), jnp.bfloat16)], axis=0
    )
    inputs_pad = jnp.concatenate([moe_input, jnp.zeros((1, columns), jnp.bfloat16)], axis=0)
    send_in = jnp.take(inputs_pad, slot_token, axis=0).reshape(sp_count, capacity, columns)
    send_grad = jnp.take(weighted_pad, slot_pair, axis=0).reshape(sp_count, capacity, columns)
    recv_in, recv_grad = (
        lax.all_to_all(send_in, "sp", split_axis=0, concat_axis=0, tiled=True),
        lax.all_to_all(send_grad, "sp", split_axis=0, concat_axis=0, tiled=True),
    )
    rows_in, rows_grad = (
        lax.all_gather(recv_in.reshape(row_total, -1), "tp", axis=1, tiled=True),
        gathered_columns(recv_grad.reshape(row_total, -1)),
    )
    key_rows, value_rows, log_decay, recv_in = lax.optimization_barrier(
        (key_rows, value_rows, log_decay, recv_in)
    )
    width, values = (key_rows.shape[1], value_rows.shape[1])
    work = token_count * values * (width + values)
    span = local_call(
        span_kernel, jax.ShapeDtypeStruct((BLOCK + LOG_ROWS, width), jnp.bfloat16), 8 * work
    )(key_rows, value_rows, log_decay)
    spans = lax.all_gather(span, "sp")
    span_logs = jnp.sum(spans[:, BLOCK : BLOCK + 3].astype(jnp.float32), axis=1)
    state_in = carried_in(span_logs, spans[:, :BLOCK], False)
    mixer_out = local_call(
        mixer_kernel, jax.ShapeDtypeStruct((token_count, values), jnp.bfloat16), 16 * work
    )(queries, key_rows, value_rows, log_decay, state_in)
    rows_grad, mixer_out = lax.optimization_barrier((rows_grad, mixer_out))
    gate_weight = w_gate[0]
    up_weight = w_up[0]
    down_weight = w_down[0]
    gate_pre = jnp.dot(rows_in, gate_weight, preferred_element_type=jnp.float32)
    up_pre = jnp.dot(rows_in, up_weight, preferred_element_type=jnp.float32)
    sigmoid_gate = jax.nn.sigmoid(gate_pre)
    activated = gate_pre * sigmoid_gate
    hidden = (activated * up_pre).astype(jnp.bfloat16)
    hidden_grad = lax.dot_general(
        rows_grad, down_weight, (((1,), (1,)), ((), ())), preferred_element_type=jnp.float32
    )
    down_part = lax.dot_general(
        hidden, rows_grad, (((0,), (0,)), ((), ())), preferred_element_type=jnp.float32
    ).astype(jnp.bfloat16)
    gate_grad = (
        hidden_grad * up_pre * sigmoid_gate * (1.0 + gate_pre * (1.0 - sigmoid_gate))
    ).astype(jnp.bfloat16)
    up_grad = (hidden_grad * activated).astype(jnp.bfloat16)
    gate_part = lax.dot_general(
        rows_in, gate_grad, (((0,), (0,)), ((), ())), preferred_element_type=jnp.float32
    ).astype(jnp.bfloat16)
    up_part = lax.dot_general(
        rows_in, up_grad, (((0,), (0,)), ((), ())), preferred_element_type=jnp.float32
    ).astype(jnp.bfloat16)
    partial_value = lax.dot_general(
        gate_grad, gate_weight, (((1,), (1,)), ((), ())), preferred_element_type=jnp.float32
    )
    partial_value = partial_value + lax.dot_general(
        up_grad, up_weight, (((1,), (1,)), ((), ())), preferred_element_type=jnp.float32
    )
    row_part = scattered_columns(partial_value.astype(jnp.bfloat16))
    row_part, gate_part, up_part, down_part = lax.optimization_barrier(
        (row_part, gate_part, up_part, down_part)
    )
    back_rows = lax.all_to_all(
        row_part.reshape(sp_count, capacity, -1), "sp", split_axis=0, concat_axis=0, tiled=True
    ).reshape(row_total, -1)
    routed = jnp.sum(
        jnp.take(back_rows, pair_slot, axis=0).astype(jnp.float32).reshape(token_count, TOP, -1),
        axis=1,
    )
    residual_grad = (out_grad.astype(jnp.float32) + routed).astype(jnp.bfloat16)
    full_grad = gathered_columns(residual_grad)
    grad_proj = lax.psum_scatter(
        lax.dot_general(
            full_grad, mixer_out, (((0,), (0,)), ((), ())), preferred_element_type=jnp.float32
        ).astype(jnp.bfloat16),
        "sp",
        scatter_dimension=0,
        tiled=True,
    ).astype(jnp.float32)
    mixer_grad = jnp.dot(full_grad, w_out, preferred_element_type=jnp.float32).astype(jnp.bfloat16)
    span_grad = local_call(
        span_grad_kernel, jax.ShapeDtypeStruct((BLOCK, width), jnp.bfloat16), 8 * work
    )(queries, log_decay, mixer_grad)
    span_grads = lax.all_gather(span_grad, "sp")
    state_out_grad = carried_in(span_logs, span_grads, True)
    query_grad, key_grad, value_grad, decay_grad = local_call(
        mixer_grad_kernel,
        (
            jax.ShapeDtypeStruct(queries.shape, jnp.bfloat16),
            jax.ShapeDtypeStruct(key_rows.shape, jnp.bfloat16),
            jax.ShapeDtypeStruct(value_rows.shape, jnp.bfloat16),
            jax.ShapeDtypeStruct(log_decay.shape, jnp.float32),
        ),
        32 * work,
        [pltpu.VMEM((token_count // BLOCK, values, width), jnp.float32)],
    )(queries, key_rows, value_rows, log_decay, mixer_grad, state_in, state_out_grad)
    return (
        gate_part[None],
        up_part[None],
        down_part[None],
        grad_proj,
        query_grad,
        key_grad,
        value_grad,
        decay_grad,
    )


def solution(mesh):
    in_specs = (
        P("sp", "tp"),
        P("sp", "tp"),
        P("sp", None),
        P("sp", None),
        P("sp", None, "tp"),
        P("sp", None, "tp"),
        P("sp", "tp", None),
        P(None, "tp"),
        P("sp", "tp"),
        P("sp", "tp"),
        P("sp", "tp"),
        P("sp", "tp"),
    )
    out_specs = (
        P("sp", None, "tp"),
        P("sp", None, "tp"),
        P("sp", "tp", None),
        P("sp", "tp"),
        P("sp", "tp"),
        P("sp", "tp"),
        P("sp", "tp"),
        P("sp", "tp"),
    )
    return jax.shard_map(body, mesh=mesh, in_specs=in_specs, out_specs=out_specs, check_vma=False)
```
